32 devices in a mesh: sp: 8 (over z, x), dp: 4 (over y, core).
Axes of the slice: x: 2, y: 2, z: 4, core: 2. Of those that a mesh axis runs over, the one named last changes fastest.
Arguments:
- stream: bfloat16 [4, 1536, 2048], P('dp', 'sp'), may hold values from -6 to 6
- queries: bfloat16 [4, 1536, 2048], P('dp', 'sp'), may hold values from -6 to 6
- key_rows: bfloat16 [4, 1536, 2048], P('dp', 'sp'), may hold values from -6 to 6
- value_rows: bfloat16 [4, 1536, 4096], P('dp', 'sp'), may hold values from -6 to 6
- input_gate: bfloat16 [4, 1536, 16], P('dp', 'sp'), may hold values from -4 to 206
- forget_gate: bfloat16 [4, 1536, 16], P('dp', 'sp'), may hold values from 0 to 12
- head_gain: float32 [16, 256], P('sp'), may hold values from 0.1 to 1.9
- out_weight: bfloat16 [4096, 2048], P('sp'), may hold values from -0.09375 to 0.09375
- mix_gain: float32 [2048], replicated, may hold values from 0.1 to 1.9
- ffn_gain: float32 [2048], replicated, may hold values from 0.1 to 1.9
- final_gain: float32 [2048], replicated, may hold values from 0.1 to 1.9
- expert_ids: int32 [4, 1536, 4], P('dp', 'sp'), may hold values from 0 to 31, all different within a row; in each aligned block of 192 rows (0 to 191, 192 to 383, ..., all dimensions but the last counted through in order) at most 36 rows name the same one
- route_scores: float32 [4, 1536, 4], P('dp', 'sp'), may hold values from 0.05 to 1
- expert_gate: bfloat16 [32, 2048, 512], P(('sp', 'dp')), may hold values from -0.125 to 0.125
- expert_up: bfloat16 [32, 2048, 512], P(('sp', 'dp')), may hold values from -0.125 to 0.125
- expert_down: bfloat16 [32, 512, 2048], P(('sp', 'dp')), may hold values from -0.25 to 0.25
- shared_gate: bfloat16 [2048, 512], replicated, may hold values from -0.125 to 0.125
- shared_up: bfloat16 [2048, 512], replicated, may hold values from -0.125 to 0.125
- shared_down: bfloat16 [512, 2048], replicated, may hold values from -0.25 to 0.25
Outputs:
- updated: bfloat16 [4, 1536, 2048], P('dp', 'sp')
The draws below stay inside these ranges and needn't reach their ends.
Inputs may be any that keep to these rules, and one draw needn't show every extreme that they name: `expert_ids`: each token names 4 different experts. Among the tokens of one device no expert is named by more than 36 tokens, a bound that some block reaches of some device.
All inputs are finite; a program needn't handle non-finite values.
Results may differ from the reference program's by a relative error of at most 0.006.
Values may be sent and summed in bfloat16 or wider, within the bound.
No kernel may reach another device: no remote copies, remote signals or barrier semaphores. Data moves between devices by JAX's collectives and lax.ppermute only.
A program may use at most 128 MiB of HBM per device.

```python
import math
import jax
import jax.numpy as jnp
import numpy as np
from jax import lax

D = 2048
HEADS = 16
QK = 128
VD = 256
FF = 512
SHARED_FF = 512
TOPK = 4
BLOCK = 256
TOK_DEV = 192
SEQUENCE_COUNT = 4
SEQUENCE_LENGTH = 1536
EXPERTS = 32
CAP = 36


def draw_forget_gate(key, part):
    random_subkeys = jax.random.split(jax.random.fold_in(key, 11), 7)
    fast_share = 0.5
    fast_heads = jax.random.uniform(random_subkeys[0], (SEQUENCE_COUNT, 1, HEADS)) < fast_share
    slow_rate = jax.random.uniform(random_subkeys[1], (SEQUENCE_COUNT, 1, HEADS), minval=0.3, maxval=2.0) / SEQUENCE_LENGTH
    fast_rate = jnp.exp(jax.random.uniform(random_subkeys[2], (SEQUENCE_COUNT, 1, HEADS), minval=math.log(1.0 / 100.0), maxval=math.log(1.0 / 30.0)))
    decay_rate = jnp.where(fast_heads, fast_rate, slow_rate)
    blocks = SEQUENCE_LENGTH // TOK_DEV
    factor = jnp.exp(jax.random.uniform(random_subkeys[3], (SEQUENCE_COUNT, blocks, 1), minval=math.log(0.5), maxval=math.log(2.0)))
    factor = jnp.repeat(factor, TOK_DEV, axis=1)
    jitter = jax.random.uniform(random_subkeys[4], (SEQUENCE_COUNT, SEQUENCE_LENGTH, HEADS), minval=-1.0, maxval=1.0)
    sampled_values = -jnp.log(decay_rate * factor) + jitter
    spike_locations = jax.random.randint(random_subkeys[5], (SEQUENCE_COUNT, 3), 0, SEQUENCE_LENGTH)
    position_lookup = jnp.arange(SEQUENCE_LENGTH)[None, None, :]
    spike_matched = jnp.any(position_lookup == spike_locations[:, :, None], axis=1)[:, :, None]
    retained_entries = jax.random.uniform(random_subkeys[6], (SEQUENCE_COUNT, SEQUENCE_LENGTH, HEADS), minval=0.5, maxval=0.8)
    spike_factor = jnp.log(retained_entries / (1.0 - retained_entries))
    sampled_values = jnp.clip(jnp.where(spike_matched, spike_factor, sampled_values), 0.0, 12.0)
    return sampled_values.astype(jnp.bfloat16)


def draw_input_gate(key, part):
    random_subkeys = jax.random.split(jax.random.fold_in(key, 23), 1)
    sampled_values = jnp.clip(jax.random.normal(random_subkeys[0], (SEQUENCE_COUNT, SEQUENCE_LENGTH, HEADS)), -4.0, 4.0)
    return sampled_values.astype(jnp.bfloat16)


def steps_of(rng, dims, cuts, least, high):
    def one(position, shards_of):
        heights = jax.random.uniform(jax.random.fold_in(jax.random.fold_in(rng, 6), position), (shards_of,), jnp.float32, least / len(cuts), high / len(cuts))
        return jnp.repeat(jnp.exp(heights), dims[position] // shards_of).reshape((-1,) + (1,) * (len(dims) - position - 1))

    level = one(*cuts[0])
    for cut in cuts[1:]:
        level = level * one(*cut)
    return level


def routed_block(stream_key, own, number, rows, number_of, top, reach, slope):
    sequence = jax.random.permutation(stream_key, number_of)
    crowded, usual = load_shares(number_of, rows * top, reach, slope, True), load_shares(number_of, rows * top, reach, slope, False)
    places = jnp.arange(number_of)

    def named(sizes, turn):
        used = int((sizes > 0).sum())
        fixed = max(1, used // 4)
        moved = fixed + (places - fixed + turn * (used - fixed)) % max(1, number_of - fixed)
        return jnp.zeros((number_of,), jnp.int32).at[sequence[jnp.where(places < fixed, places, moved)]].set(jnp.asarray(sizes, jnp.int32))

    sizes = jnp.where(number % 4 == 0, named(crowded, number // 4), named(usual, number - number // 4 - 1))
    mixed = jax.random.permutation(jax.random.fold_in(own, 3), number_of)
    donor, sink = mixed[0:number_of // 2 * 2:2], mixed[1:number_of // 2 * 2:2]
    margin = jnp.minimum(sizes[donor] - 1, reach - sizes[sink]) // 2
    margin = jnp.where((donor == sequence[0]) | (sink == sequence[0]) | (sizes[sink] == 0), 0, jnp.maximum(margin, 0))
    moved = jax.random.randint(jax.random.fold_in(own, 4), (number_of // 2,), 0, 1 << 20) % (margin + 1)
    sizes = sizes.at[donor].add(-moved).at[sink].add(moved)
    labels = jnp.searchsorted(jnp.cumsum(sizes), jnp.arange(rows * top), side="right").astype(jnp.int32)
    listing = labels.reshape(top, rows).T
    listing = listing[jax.random.permutation(jax.random.fold_in(own, 1), rows)]
    turn = jax.random.randint(jax.random.fold_in(own, 2), (rows, 1), 0, top)
    return jnp.take_along_axis(listing, (jnp.arange(top)[None, :] + turn) % top, axis=1)


def load_shares(amount, total, bound, skew, full):
    portions = [(1 << 20) // math.isqrt(rank ** skew) + 1 for rank in range(1, amount + 1)]
    largest = bound if full else min(bound, max(-(-total // amount), total * portions[0] // sum(portions)))
    least = 1 if total - largest >= amount - 1 else 0
    holding, spare = [largest] + [least] * (amount - 1), total - largest - least * (amount - 1)
    while spare > 0:
        candidates = [i for i in range(1, amount) if holding[i] < largest] or [i for i in range(1, amount) if holding[i] < bound]
        whole, remaining = sum([portions[i] for i in candidates]), spare
        for i in candidates:
            extra = min(bound - holding[i], max(1, remaining * portions[i] // whole), spare)
            holding[i] = holding[i] + extra
            spare = spare - extra
    return np.array(holding)


def noise(rng, extent, deviation, reach, cuts=(), kind=jnp.bfloat16):
    values = deviation * jax.random.normal(rng, extent, jnp.float32)
    if cuts:
        values = values * steps_of(rng, extent, cuts, -0.22, 0.18)
    return jnp.clip(values, -reach, reach).astype(kind)


def setup_inputs(seed: int = 0) -> dict:
    arg_keys = jax.random.split(jax.random.key(seed), 20)
    stream = noise(arg_keys[0], (SEQUENCE_COUNT, SEQUENCE_LENGTH, D), 1.0, 6.0, ((0, 4), (1, 8)))
    queries = noise(arg_keys[1], (SEQUENCE_COUNT, SEQUENCE_LENGTH, HEADS * QK), 1.0, 6.0, ((0, 4), (1, 8)))
    key_rows = noise(arg_keys[2], (SEQUENCE_COUNT, SEQUENCE_LENGTH, HEADS * QK), 1.0, 6.0, ((0, 4), (1, 8)))
    value_rows = noise(arg_keys[3], (SEQUENCE_COUNT, SEQUENCE_LENGTH, HEADS * VD), 1.0, 6.0, ((0, 4), (1, 8)))
    input_gate = draw_input_gate(jax.random.fold_in(arg_keys[19], 71), 0)
    forget_gate = draw_forget_gate(jax.random.fold_in(arg_keys[19], 71), 0)
    head_gain = jnp.clip(1.0 + 0.18 * jax.random.normal(arg_keys[6], (HEADS, VD), jnp.float32), 0.1, 1.9)
    out_weight = noise(arg_keys[7], (HEADS * VD, D), (HEADS * VD) ** -0.5, 0.09375, ((0, 8),))
    mix_gain = jnp.clip(1.0 + 0.18 * jax.random.normal(arg_keys[8], (D,), jnp.float32), 0.1, 1.9)
    ffn_gain = jnp.clip(1.0 + 0.18 * jax.random.normal(arg_keys[9], (D,), jnp.float32), 0.1, 1.9)
    final_gain = jnp.clip(1.0 + 0.18 * jax.random.normal(arg_keys[10], (D,), jnp.float32), 0.1, 1.9)
    expert_ids_keys = jax.random.split(jax.random.fold_in(arg_keys[11], 1), SEQUENCE_COUNT * SEQUENCE_LENGTH // TOK_DEV)
    expert_ids_turns = jax.random.permutation(jax.random.fold_in(arg_keys[11], 3), SEQUENCE_COUNT * SEQUENCE_LENGTH // TOK_DEV)
    expert_ids = jax.vmap(lambda own, number: routed_block(jax.random.fold_in(arg_keys[11], 2), own, number, TOK_DEV, EXPERTS, TOPK, CAP, 2))(expert_ids_keys, expert_ids_turns).reshape((SEQUENCE_COUNT, SEQUENCE_LENGTH, TOPK))
    route_scores = jnp.clip(0.05 + 0.95 * jax.random.uniform(arg_keys[12], (SEQUENCE_COUNT, SEQUENCE_LENGTH, TOPK), jnp.float32) ** steps_of(arg_keys[12], (SEQUENCE_COUNT, SEQUENCE_LENGTH, TOPK), ((0, 4), (1, 8)), -0.2, 0.2), 0.05, 1.0)
    expert_gate = noise(arg_keys[13], (EXPERTS, D, FF), D ** -0.5, 0.125, ((0, 32),))
    expert_up = noise(arg_keys[14], (EXPERTS, D, FF), D ** -0.5, 0.125, ((0, 32),))
    expert_down = noise(arg_keys[15], (EXPERTS, FF, D), FF ** -0.5, 0.25, ((0, 32),))
    shared_gate = noise(arg_keys[16], (D, SHARED_FF), D ** -0.5, 0.125)
    shared_up = noise(arg_keys[17], (D, SHARED_FF), D ** -0.5, 0.125)
    shared_down = noise(arg_keys[18], (SHARED_FF, D), SHARED_FF ** -0.5, 0.25)
    return dict(stream=stream, queries=queries, key_rows=key_rows, value_rows=value_rows, input_gate=input_gate, forget_gate=forget_gate, head_gain=head_gain, out_weight=out_weight, mix_gain=mix_gain, ffn_gain=ffn_gain, final_gain=final_gain, expert_ids=expert_ids, route_scores=route_scores, expert_gate=expert_gate, expert_up=expert_up, expert_down=expert_down, shared_gate=shared_gate, shared_up=shared_up, shared_down=shared_down)


EPSILON = 1e-06
ROUTE_BOOST = 2.5
HIGHEST = lax.Precision.HIGHEST

def root_norm(values, gains):
    return values * lax.rsqrt(lax.optimization_barrier(jnp.mean(values * values, axis=-1, keepdims=True)) + EPSILON) * gains

def cell_block(carry, pieces):
    state, normal, stabilizer = carry
    query_part, key_part, value_part, gate_part, decay_part = pieces
    length = query_part.shape[1]
    causal = jnp.tril(jnp.ones((length, length), dtype=bool))
    cumulative = jnp.cumsum(decay_part, axis=-1)
    logits = jnp.where(causal[None], cumulative[:, :, None] - cumulative[:, None, :] + gate_part[:, None, :], -jnp.inf)
    peak = jnp.maximum(cumulative + stabilizer[:, None], lax.optimization_barrier(jnp.max(logits, axis=-1)))
    weights = jnp.exp(logits - peak[:, :, None])
    scores = jnp.einsum('hld,hsd->hls', query_part, key_part, precision=HIGHEST) * weights
    carried = jnp.exp(cumulative + stabilizer[:, None] - peak)
    numerator = jnp.einsum('hls,hsv->hlv', scores, value_part, precision=HIGHEST) + carried[:, :, None] * jnp.einsum('hvd,hld->hlv', state, query_part, precision=HIGHEST)
    denominator = lax.optimization_barrier(jnp.sum(scores, axis=-1)) + carried * jnp.einsum('hd,hld->hl', normal, query_part, precision=HIGHEST)
    result = numerator / jnp.maximum(jnp.abs(denominator), jnp.exp(-peak))[:, :, None]
    block_end = cumulative[:, -1]
    write_log = block_end[:, None] - cumulative + gate_part
    peak_next = jnp.maximum(block_end + stabilizer, lax.optimization_barrier(jnp.max(write_log, axis=-1)))
    decay_all = jnp.exp(block_end + stabilizer - peak_next)
    written = jnp.exp(write_log - peak_next[:, None])[:, :, None] * key_part
    state = decay_all[:, None, None] * state + jnp.einsum('hlv,hld->hvd', value_part, written, precision=HIGHEST)
    normal = decay_all[:, None] * normal + lax.optimization_barrier(jnp.sum(written, axis=1))
    return ((state, normal, peak_next), result)

def memory_cell(queries, key_rows, value_rows, input_gate, forget_gate):
    length, head_count = (queries.shape[0], queries.shape[1])
    key_width = queries.shape[2]
    value_width = value_rows.shape[2]
    blocks = length // BLOCK

    def to_blocks(tensor):
        shaped = tensor.astype(jnp.float32).reshape((blocks, BLOCK, head_count) + tensor.shape[2:])
        return jnp.moveaxis(shaped, 2, 1)
    decay_log = jax.nn.log_sigmoid(forget_gate.astype(jnp.float32))
    start_state = (jnp.zeros((head_count, value_width, key_width), jnp.float32), jnp.zeros((head_count, key_width), jnp.float32), jnp.zeros((head_count,), jnp.float32))
    pieces = (to_blocks(queries), to_blocks(key_rows) * key_width ** (-0.5), to_blocks(value_rows), to_blocks(input_gate), to_blocks(decay_log))
    _, outputs = lax.scan(cell_block, start_state, pieces)
    return jnp.moveaxis(outputs, 1, 2).reshape(length, head_count, value_width)

def reference(stream, queries, key_rows, value_rows, input_gate, forget_gate, head_gain, out_weight, mix_gain, ffn_gain, final_gain, expert_ids, route_scores, expert_gate, expert_up, expert_down, shared_gate, shared_up, shared_down):
    seq_count, length, model_width = stream.shape
    head_count = head_gain.shape[0]

    def one_sequence(sequence_arrays):
        return memory_cell(sequence_arrays[0].reshape(length, head_count, -1), sequence_arrays[1].reshape(length, head_count, -1), sequence_arrays[2].reshape(length, head_count, -1), sequence_arrays[3], sequence_arrays[4])
    cell_out = lax.map(one_sequence, (queries, key_rows, value_rows, input_gate, forget_gate))
    normed = root_norm(cell_out, head_gain).astype(jnp.bfloat16).reshape(seq_count * length, -1)
    mixer_out = jnp.dot(normed, out_weight, preferred_element_type=jnp.float32)
    residual = stream.reshape(-1, model_width).astype(jnp.float32) + root_norm(mixer_out, mix_gain)
    ffn_input = root_norm(residual, ffn_gain).astype(jnp.bfloat16)
    shared_hidden = (jax.nn.silu(jnp.dot(ffn_input, shared_gate, preferred_element_type=jnp.float32)) * jnp.dot(ffn_input, shared_up, preferred_element_type=jnp.float32)).astype(jnp.bfloat16)
    shared_out = jnp.dot(shared_hidden, shared_down, preferred_element_type=jnp.float32)
    token_total = seq_count * length
    top_count = expert_ids.shape[2]
    expert_count = expert_gate.shape[0]
    blocks = token_total // TOK_DEV
    route_ids = expert_ids.reshape(blocks, TOK_DEV * top_count).astype(jnp.int32)
    chosen = (route_ids[:, :, None] == jnp.arange(expert_count, dtype=jnp.int32)[None, None, :]).astype(jnp.int32)
    before = lax.optimization_barrier(jnp.sum((jnp.cumsum(chosen, axis=1) - chosen) * chosen, axis=2))
    block_ids = jnp.arange(blocks, dtype=jnp.int32)[:, None]
    slot_index = ((route_ids * blocks + block_ids) * CAP + before).astype(jnp.int32)
    slot_owner = jnp.full((expert_count * blocks * CAP,), -1, jnp.int32)
    slot_owner = slot_owner.at[slot_index.reshape(-1)].set(jnp.arange(token_total * top_count, dtype=jnp.int32))
    slot_owner = slot_owner.reshape(expert_count, blocks * CAP)
    scores = route_scores.reshape(token_total, top_count).astype(jnp.float32)
    route_share = (scores / lax.optimization_barrier(jnp.sum(scores, axis=1, keepdims=True)) * ROUTE_BOOST).reshape(-1)

    def expert_step(routed, expert_arrays):
        owners, gate_w, up_w, down_w = expert_arrays
        filled = owners >= 0
        source = jnp.where(filled, owners, 0).astype(jnp.int32)
        token_rows = (source // top_count).astype(jnp.int32)
        picked = jnp.where(filled[:, None], ffn_input[token_rows], jnp.zeros((), jnp.bfloat16))
        hidden = (jax.nn.silu(jnp.dot(picked, gate_w, preferred_element_type=jnp.float32)) * jnp.dot(picked, up_w, preferred_element_type=jnp.float32)).astype(jnp.bfloat16)
        answer = jnp.dot(hidden, down_w, preferred_element_type=jnp.float32).astype(jnp.bfloat16)
        answer = lax.optimization_barrier(answer).astype(jnp.float32)
        weighted = answer * jnp.where(filled, route_share[source], 0.0)[:, None]
        return (routed.at[token_rows].add(weighted), None)
    routed, _ = lax.scan(expert_step, jnp.zeros((token_total, model_width), jnp.float32), (slot_owner, expert_gate, expert_up, expert_down))
    moe_total = routed + shared_out
    updated = residual + root_norm(moe_total, final_gain)
    return updated.astype(jnp.bfloat16).reshape(seq_count, length, model_width)
```

```python
import functools

import jax
import jax.numpy as jnp
from jax import lax
from jax.experimental import pallas as pl
from jax.experimental.pallas import tpu as pltpu
from jax.sharding import PartitionSpec as P

EPSILON = 1e-06
ROUTE_BOOST = 2.5
HIGHEST = lax.Precision.HIGHEST
ROWS_BY_ROWS = (((0,), (0,)), ((), ()))
LANES_BY_LANES = (((1,), (1,)), ((), ()))


def root_norm(values, gains):
    return values * lax.rsqrt(jnp.mean(values * values, axis=-1, keepdims=True) + EPSILON) * gains


def split_parts(values, count):
    parts = []
    for _ in range(count):
        part = lax.reduce_precision(values, 8, 7)
        parts.append(part.astype(jnp.bfloat16))
        values = values - part
    return parts


def kernel_parts(values, count):
    parts = []
    for _ in range(count):
        parts.append(values.astype(jnp.bfloat16))
        values = values - parts[-1].astype(jnp.float32)
    return parts


def mxu(left, right, dims=(((1,), (0,)), ((), ()))):
    return lax.dot_general(left, right, dims, preferred_element_type=jnp.float32)


def column_of(table, head):
    lanes = lax.broadcasted_iota(jnp.int32, table.shape, 1)
    return jnp.sum(jnp.where(lanes == head, table, 0.0), axis=1, keepdims=True)


def write_states(k_ref, v_ref, source_ref, state_ref, normal_ref, *, group, qk, vd):
    for j in range(group):
        head = pl.program_id(0) * group + j
        source = column_of(source_ref[...], head)
        top = jnp.max(source, axis=0, keepdims=True)
        keys = k_ref[:, j * qk : (j + 1) * qk].astype(jnp.float32) * qk ** (-0.5)
        written = jnp.exp(source - top) * keys
        values = v_ref[:, j * vd : (j + 1) * vd]
        state_ref[j] = sum(mxu(part, values, ROWS_BY_ROWS) for part in kernel_parts(written, 3))
        normal_ref[j] = jnp.sum(written, axis=0, keepdims=True)


def chain_states(place_ref, stats_ref, written_ref, prefix_ref, entry_ref, *, steps, mine, heads, qk):
    place = place_ref[0]
    for j in range(mine):
        state = jnp.zeros(written_ref.shape[2:], jnp.float32)
        level = jnp.zeros((1, 1), jnp.float32)
        for t in range(steps):
            prefix_ref[t, j] = state
            row = stats_ref[t, pl.ds(place * mine + j, 1), :]
            top, fall = row[:, qk : qk + 1], row[:, qk + 1 : qk + 2]
            peak = jnp.maximum(level, top)
            state = jnp.exp(level - peak) * state + jnp.exp(top - peak) * written_ref[t, j]
            level = fall + peak
    normal = jnp.zeros((heads, qk), jnp.float32)
    level = jnp.zeros((heads, 1), jnp.float32)
    for t in range(steps):
        table = stats_ref[t, :heads, :]
        top, fall = table[:, qk : qk + 1], table[:, qk + 1 : qk + 2]
        peak = jnp.maximum(level, top)
        grown = jnp.exp(level - peak) * normal + jnp.exp(top - peak) * table[:, :qk]
        normal = jnp.where(t < place, grown, normal)
        level = jnp.where(t < place, fall + peak, level)
    entry_ref[:, :qk] = normal
    entry_ref[:, qk:] = jnp.broadcast_to(level, (heads, entry_ref.shape[1] - qk))


def read_cells(q_ref, k_ref, v_ref, total_ref, row_ref, prefix_ref, entry_ref, gain_ref, out_ref, *, group, qk, vd):
    length = q_ref.shape[0]
    rows = lax.broadcasted_iota(jnp.int32, (length, length), 0)
    lanes = lax.broadcasted_iota(jnp.int32, (length, length), 1)
    for j in range(group):
        head = pl.program_id(0) * group + j
        total = column_of(total_ref[...], head)
        source = jnp.where(lanes <= rows, row_ref[0, j : j + 1, :], -jnp.inf)
        level = entry_ref[0, j : j + 1, qk : qk + 1]
        normal = entry_ref[0, j : j + 1, :qk]
        peak = jnp.maximum(jnp.max(source, axis=1, keepdims=True), level)
        query = q_ref[:, j * qk : (j + 1) * qk]
        values = v_ref[:, j * vd : (j + 1) * vd]
        scores = mxu(query, k_ref[:, j * qk : (j + 1) * qk], LANES_BY_LANES) * qk ** (-0.5)
        scores = scores * jnp.exp(source - peak)
        carried = jnp.exp(level - peak)
        numerator = sum(mxu(part, values) for part in kernel_parts(scores, 3)) + carried * sum(
            mxu(query, part) for part in kernel_parts(prefix_ref[j], 3)
        )
        denominator = jnp.sum(scores, axis=1, keepdims=True) + carried * jnp.sum(
            query.astype(jnp.float32) * normal, axis=1, keepdims=True
        )
        cell = numerator / jnp.maximum(jnp.abs(denominator), jnp.exp(-(total + peak)))
        out_ref[:, j * vd : (j + 1) * vd] = root_norm(cell, gain_ref[0, j : j + 1, :]).astype(jnp.bfloat16)


def cell_rows(queries, key_rows, value_rows, input_gate, forget_gate, head_gain):
    steps = lax.axis_size("sp")
    place = lax.axis_index("sp")
    mine, vd = head_gain.shape
    length, heads = input_gate.shape
    qk = queries.shape[1] // heads
    group = 4 if heads % 4 == 0 else 1
    blocks = heads // group
    decay = jax.nn.log_sigmoid(forget_gate.astype(jnp.float32))
    lower = jnp.tril(jnp.ones((length, length), jnp.float32))
    total = jnp.dot(lower, decay, precision=HIGHEST)
    source = input_gate.astype(jnp.float32) - total

    def lanes_of(width):
        return pl.BlockSpec((length, group * width), lambda i: (0, i))

    table = pl.BlockSpec((length, heads), lambda i: (0, 0))
    written, normals = pl.pallas_call(
        functools.partial(write_states, group=group, qk=qk, vd=vd),
        grid=(blocks,),
        in_specs=[lanes_of(qk), lanes_of(vd), table],
        out_specs=[
            pl.BlockSpec((group, qk, vd), lambda i: (i, 0, 0)),
            pl.BlockSpec((group, 1, qk), lambda i: (i, 0, 0)),
        ],
        out_shape=[
            jax.ShapeDtypeStruct((heads, qk, vd), jnp.float32),
            jax.ShapeDtypeStruct((heads, 1, qk), jnp.float32),
        ],
        name="write_states",
    )(key_rows, value_rows, source)
    stats = jnp.concatenate(
        [
            normals[:, 0],
            jnp.max(source, axis=0)[:, None],
            total[-1][:, None],
            jnp.zeros((heads, vd - qk - 2), jnp.float32),
        ],
        axis=1,
    )
    stats = lax.all_gather(jnp.concatenate([stats, head_gain], axis=0), "sp", axis=0)
    gains = stats[:, heads:].reshape(blocks, group, vd)
    arrived = lax.all_to_all(written.reshape(steps, mine, qk, vd), "sp", split_axis=0, concat_axis=0, tiled=True)
    whole = pl.BlockSpec(memory_space=pltpu.VMEM)
    prefixes, entry = pl.pallas_call(
        functools.partial(chain_states, steps=steps, mine=mine, heads=heads, qk=qk),
        in_specs=[pl.BlockSpec(memory_space=pltpu.SMEM), whole, whole],
        out_specs=[whole, whole],
        out_shape=[
            jax.ShapeDtypeStruct((steps, mine, qk, vd), jnp.float32),
            jax.ShapeDtypeStruct((heads, 2 * qk), jnp.float32),
        ],
        name="chain_states",
    )(place.reshape(1).astype(jnp.int32), stats, arrived)
    prefixes = lax.all_to_all(prefixes, "sp", split_axis=0, concat_axis=0, tiled=True)
    row = pl.BlockSpec((1, group, length), lambda i: (i, 0, 0))
    return pl.pallas_call(
        functools.partial(read_cells, group=group, qk=qk, vd=vd),
        grid=(blocks,),
        in_specs=[
            lanes_of(qk),
            lanes_of(qk),
            lanes_of(vd),
            table,
            row,
            pl.BlockSpec((group, qk, vd), lambda i: (i, 0, 0)),
            pl.BlockSpec((1, group, 2 * qk), lambda i: (i, 0, 0)),
            pl.BlockSpec((1, group, vd), lambda i: (i, 0, 0)),
        ],
        out_specs=lanes_of(vd),
        out_shape=jax.ShapeDtypeStruct((length, heads * vd), jnp.bfloat16),
        name="read_cells",
    )(
        queries,
        key_rows,
        value_rows,
        total,
        source.T.reshape(blocks, group, length),
        prefixes.reshape(heads, qk, vd),
        entry.reshape(blocks, group, 2 * qk),
        gains,
    )


def gather_rows(weight):
    share = weight.shape[0] // lax.axis_size("dp")
    piece = lax.dynamic_slice_in_dim(weight, lax.axis_index("dp") * share, share, 0)
    return lax.all_gather(piece, ("sp", "dp"), axis=0, tiled=True)


def local(
    stream,
    queries,
    key_rows,
    value_rows,
    input_gate,
    forget_gate,
    head_gain,
    out_weight,
    mix_gain,
    ffn_gain,
    final_gain,
    expert_ids,
    route_scores,
    expert_gate,
    expert_up,
    expert_down,
    shared_gate,
    shared_up,
    shared_down,
):
    token_count = stream.shape[1]
    model_width = stream.shape[2]
    gathered_weight = gather_rows(out_weight)
    normed = cell_rows(
        queries[0], key_rows[0], value_rows[0], input_gate[0], forget_gate[0], head_gain
    )
    mixer_out = jnp.dot(normed, gathered_weight, preferred_element_type=jnp.float32)
    residual = stream[0].astype(jnp.float32) + root_norm(mixer_out, mix_gain)
    ffn_input = root_norm(residual, ffn_gain).astype(jnp.bfloat16)
    top_count = expert_ids.shape[2]
    local_count = expert_gate.shape[0]
    expert_count = lax.axis_size("sp") * lax.axis_size("dp") * local_count
    capacity = max(2, 3 * token_count * top_count // (2 * expert_count))
    capacity = -(-capacity // 8) * 8
    ids = expert_ids[0]
    named = ids[:, :, None] == jnp.arange(expert_count, dtype=jnp.int32)[None, None, :]
    chosen = jnp.any(named, axis=1).astype(jnp.bfloat16)
    earlier = jnp.tril(jnp.ones((token_count, token_count), jnp.bfloat16), -1)
    rank = jnp.dot(earlier, chosen, preferred_element_type=jnp.float32).astype(jnp.int32)
    before = jnp.sum(jnp.where(named, rank[:, None, :], 0), axis=2)
    slot_index = ids * capacity + before
    slots = jnp.arange(expert_count * capacity, dtype=jnp.int32)[None, :]
    scores = route_scores[0]
    route_share = scores / jnp.sum(scores, axis=1, keepdims=True) * ROUTE_BOOST
    placed = jnp.zeros((token_count, expert_count * capacity), jnp.bfloat16)
    shares = jnp.zeros((token_count, expert_count * capacity), jnp.float32)
    for column in range(top_count):
        hit = slot_index[:, column][:, None] == slots
        placed = jnp.where(hit, jnp.ones((), jnp.bfloat16), placed)
        shares = jnp.where(hit, route_share[:, column][:, None], shares)
    share_high, share_low = split_parts(shares, 2)
    outgoing = mxu(placed, ffn_input, ROWS_BY_ROWS).astype(jnp.bfloat16)
    outgoing = outgoing.reshape(expert_count, capacity, model_width)
    slot_rows = lax.all_to_all(outgoing, ("sp", "dp"), split_axis=0, concat_axis=0, tiled=True)
    shaped = slot_rows.reshape(-1, local_count, slot_rows.shape[1], model_width)
    gate_proj = jnp.einsum(
        "nlcd,ldf->nlcf", shaped, expert_gate, preferred_element_type=jnp.float32
    )
    up_proj = jnp.einsum("nlcd,ldf->nlcf", shaped, expert_up, preferred_element_type=jnp.float32)
    hidden = (jax.nn.silu(gate_proj) * up_proj).astype(jnp.bfloat16)
    answer = jnp.einsum("nlcf,lfd->nlcd", hidden, expert_down, preferred_element_type=jnp.float32)
    expert_out = answer.astype(jnp.bfloat16).reshape(slot_rows.shape)
    returned = lax.all_to_all(expert_out, ("sp", "dp"), split_axis=0, concat_axis=0, tiled=True)
    answers = returned.reshape(expert_count * capacity, model_width)
    shared_hidden = (
        jax.nn.silu(jnp.dot(ffn_input, shared_gate, preferred_element_type=jnp.float32))
        * jnp.dot(ffn_input, shared_up, preferred_element_type=jnp.float32)
    ).astype(jnp.bfloat16)
    shared_out = jnp.dot(shared_hidden, shared_down, preferred_element_type=jnp.float32)
    moe_total = mxu(share_high, answers) + mxu(share_low, answers) + shared_out
    result = (residual + root_norm(moe_total, final_gain)).astype(jnp.bfloat16)
    return result[None]


def solution(mesh):
    placed = (
        P("dp", "sp", None),
        P("dp", "sp", None),
        P("dp", "sp", None),
        P("dp", "sp", None),
        P("dp", "sp", None),
        P("dp", "sp", None),
        P("sp", None),
        P("sp", None),
        P(),
        P(),
        P(),
        P("dp", "sp", None),
        P("dp", "sp", None),
        P(("sp", "dp"), None, None),
        P(("sp", "dp"), None, None),
        P(("sp", "dp"), None, None),
        P(),
        P(),
        P(),
    )
    return jax.shard_map(
        local, mesh=mesh, in_specs=placed, out_specs=P("dp", "sp", None), check_vma=False
    )
```
